32 devices in a mesh: sp: 8 (over z, x), tp: 4 (over y, core).
Axes of the slice: x: 2, y: 2, z: 4, core: 2. Of those that a mesh axis runs over, the one named last changes fastest.
Arguments:
- stream_in: bfloat16 [1024, 2048], P('sp'), may hold values from -8 to 8
- out_cot: bfloat16 [1024, 2048], P('sp'), may hold values from -6 to 6
- route_experts: int32 [1024, 2], P('sp'), may hold values from 0 to 7, all different within a row; in each aligned block of 128 rows (0 to 127, 128 to 255, ...) at most 64 rows name the same one
- route_weights: float32 [1024, 2], P('sp'), may hold values from 0.1 to 1
- w_gate: bfloat16 [8, 2048, 2048], P('sp', None, 'tp'), may hold values from -0.125 to 0.125
- w_up: bfloat16 [8, 2048, 2048], P('sp', None, 'tp'), may hold values from -0.125 to 0.125
- w_down: bfloat16 [8, 2048, 2048], P('sp', 'tp'), may hold values from -0.125 to 0.125
- w_proj: bfloat16 [2048, 1024], P(None, 'tp'), may hold values from -0.1875 to 0.1875
- conv_value: bfloat16 [1024, 1024], P('tp', 'sp'), may hold values from -6 to 6
- conv_gate: bfloat16 [1024, 1024], P('tp', 'sp'), may hold values from -8 to 8
- conv_taps: float32 [31, 1024], P(None, 'tp'), may hold values from -1 to 1
- conv_result: bfloat16 [1024, 1024], P('tp', 'sp'), may hold values from -100 to 100
- channel_norm_gain: float32 [1024], P('tp'), may hold values from 0.1 to 1.9
Outputs:
- grad_gate: bfloat16 [8, 2048, 2048], P('sp', None, 'tp')
- grad_up: bfloat16 [8, 2048, 2048], P('sp', None, 'tp')
- grad_down: bfloat16 [8, 2048, 2048], P('sp', 'tp')
- grad_stream: bfloat16 [1024, 2048], P('sp')
- grad_proj: float32 [2048, 1024], P('sp', 'tp')
- grad_value: bfloat16 [1024, 1024], P('tp', 'sp')
- grad_gate_in: bfloat16 [1024, 1024], P('tp', 'sp')
The draws below stay inside these ranges and needn't reach their ends.
Inputs may be any that keep to these rules, and one draw needn't show every extreme that they name: `route_experts`: each row names 2 different experts; within each aligned block of 128 rows no expert is named by more than 64 rows, and at least one block reaches that bound for some expert.
All inputs are finite; a program needn't handle non-finite values.
Results may differ from the reference program's by a relative error of at most 0.025.
Values may be sent and summed in bfloat16 or wider, within the bound.
A program may use at most 64 MiB of HBM per device.

```python
import math
import jax
import jax.numpy as jnp
import numpy as np
from jax import lax

D = 2048
FF = 2048
CONV_CHANNELS = 1024
CONV_W = 31
TOP = 2
T_DEV = 128
EXPERTS = 8
TOKENS = 1024
CAP = 64
N_SP = 8
N_TP = 4


def draw_conv_result(key, part):
    first_key, second_key, third_key = jax.random.split(jax.random.fold_in(key, 17), 3)
    base = jnp.clip(jax.random.normal(first_key, (CONV_CHANNELS, TOKENS), jnp.float32), -6.0, 6.0)
    channel_pos = jnp.arange(CONV_CHANNELS, dtype=jnp.float32) / CONV_CHANNELS
    rough = jax.random.uniform(second_key, (CONV_CHANNELS, 1), jnp.float32, 0.5, 1.5)
    shift_noise = jnp.clip(jax.random.normal(third_key, (1, TOKENS), jnp.float32), -4.0, 4.0)
    scales = jnp.exp(jnp.log(3.0) * channel_pos)[:, None] * rough
    offset = shift_noise
    return (base * scales + offset).astype(jnp.bfloat16)


def spiked(values, rng, source, target, shards_of, factor):
    def block_of(dim):
        return (jnp.arange(values.shape[dim]) // (values.shape[dim] // shards_of)).reshape((-1,) + (1,) * (values.ndim - 1 - dim))

    near = jax.random.permutation(rng, shards_of)[block_of(target)]
    second = (block_of(target) + shards_of // 2) % shards_of
    return jnp.where((block_of(source) == near) | (block_of(source) == second), factor * values, values)


def steps_of(key, extent, cuts, smallest, top_value):
    def one(dim, parts):
        heights = jax.random.uniform(jax.random.fold_in(jax.random.fold_in(key, 6), dim), (parts,), jnp.float32, smallest / len(cuts), top_value / len(cuts))
        return jnp.repeat(jnp.exp(heights), extent[dim] // parts).reshape((-1,) + (1,) * (len(extent) - dim - 1))

    gain = one(*cuts[0])
    for cut in cuts[1:]:
        gain = gain * one(*cut)
    return gain


def deal_out(own_key, own, number, rows, count, top, reach, skew):
    ranking = jax.random.permutation(own_key, count)
    heavy_load, ordinary = load_shares(count, rows * top, reach, skew, True), load_shares(count, rows * top, reach, skew, False)
    places = jnp.arange(count)

    def named(sizes, turn):
        used = int((sizes > 0).sum())
        fixed = max(1, used // 4)
        moved = fixed + (places - fixed + turn * (used - fixed)) % max(1, count - fixed)
        return jnp.zeros((count,), jnp.int32).at[ranking[jnp.where(places < fixed, places, moved)]].set(jnp.asarray(sizes, jnp.int32))

    sizes = jnp.where(number % 4 == 0, named(heavy_load, number // 4), named(ordinary, number - number // 4 - 1))
    mixed = jax.random.permutation(jax.random.fold_in(own, 3), count)
    donor, sink = mixed[0:count // 2 * 2:2], mixed[1:count // 2 * 2:2]
    slack = jnp.minimum(sizes[donor] - 1, reach - sizes[sink]) // 2
    slack = jnp.where((donor == ranking[0]) | (sink == ranking[0]) | (sizes[sink] == 0), 0, jnp.maximum(slack, 0))
    moved = jax.random.randint(jax.random.fold_in(own, 4), (count // 2,), 0, 1 << 20) % (slack + 1)
    sizes = sizes.at[donor].add(-moved).at[sink].add(moved)
    labels = jnp.searchsorted(jnp.cumsum(sizes), jnp.arange(rows * top), side="right").astype(jnp.int32)
    listing = labels.reshape(top, rows).T
    listing = listing[jax.random.permutation(jax.random.fold_in(own, 1), rows)]
    turn = jax.random.randint(jax.random.fold_in(own, 2), (rows, 1), 0, top)
    return jnp.take_along_axis(listing, (jnp.arange(top)[None, :] + turn) % top, axis=1)


def load_shares(amount, total, most, lean, full):
    portions = [(1 << 20) // math.isqrt(grade ** lean) + 1 for grade in range(1, amount + 1)]
    largest = most if full else min(most, max(-(-total // amount), total * portions[0] // sum(portions)))
    least = 1 if total - largest >= amount - 1 else 0
    given, spare = [largest] + [least] * (amount - 1), total - largest - least * (amount - 1)
    while spare > 0:
        candidates = [i for i in range(1, amount) if given[i] < largest] or [i for i in range(1, amount) if given[i] < most]
        mass, budget = sum([portions[i] for i in candidates]), spare
        for i in candidates:
            more = min(most - given[i], max(1, budget * portions[i] // mass), spare)
            given[i] = given[i] + more
            spare = spare - more
    return np.array(given)


def centred(key, extent, width, most, cuts=(), kind=jnp.bfloat16):
    entries = jax.random.normal(key, extent, jnp.float32) * width
    if len(cuts) > 0:
        entries = steps_of(key, extent, cuts, -0.22, 0.18) * entries
    return jnp.clip(entries, min=-most, max=most).astype(kind)


def gaussian_with(rng, shape, deviation, most, cuts, heavy, kind=jnp.bfloat16):
    values = deviation * jax.random.normal(rng, shape, jnp.float32)
    if cuts:
        values = values * steps_of(rng, shape, cuts, -0.22, 0.18)
    return jnp.clip(spiked(values, jax.random.fold_in(rng, 3), *heavy), -most, most).astype(kind)


def setup_inputs(seed: int = 0) -> dict:
    key_list = jax.random.split(jax.random.key(seed), 14)
    stream_in = centred(key_list[0], (TOKENS, D), 1.25, 8.0, ((0, 8),))
    out_cot = gaussian_with(key_list[1], (TOKENS, D), 1.0, 6.0, ((0, 8),), (0, 1, 8, 2.0))
    route_experts_keys = jax.random.split(jax.random.fold_in(key_list[2], 1), TOKENS // T_DEV)
    route_experts_turns = jax.random.permutation(jax.random.fold_in(key_list[2], 3), TOKENS // T_DEV)
    route_experts = jax.vmap(lambda own, number: deal_out(jax.random.fold_in(key_list[2], 2), own, number, T_DEV, EXPERTS, TOP, CAP, 2))(route_experts_keys, route_experts_turns).reshape((TOKENS, TOP))
    route_weights = jnp.clip(0.1 + 0.9 * jax.random.uniform(key_list[3], (TOKENS, TOP), jnp.float32) ** steps_of(key_list[3], (TOKENS, TOP), ((0, 8),), -0.2, 0.2), 0.1, 1.0)
    w_gate = centred(key_list[4], (EXPERTS, D, FF), D ** -0.5, 0.125, ((0, 8), (2, 4)))
    w_up = centred(key_list[5], (EXPERTS, D, FF), D ** -0.5, 0.125, ((0, 8), (2, 4)))
    w_down = centred(key_list[6], (EXPERTS, FF, D), FF ** -0.5, 0.125, ((0, 8), (1, 4)))
    w_proj = centred(key_list[7], (D, CONV_CHANNELS), CONV_CHANNELS ** -0.5, 0.1875, ((1, 4),))
    conv_value = centred(key_list[8], (CONV_CHANNELS, TOKENS), 1.0, 6.0, ((0, 4), (1, 8)))
    conv_gate = centred(key_list[9], (CONV_CHANNELS, TOKENS), 1.5, 8.0, ((0, 4), (1, 8)))
    conv_taps = centred(key_list[10], (CONV_W, CONV_CHANNELS), CONV_W ** -0.5, 1.0, ((1, 4),), jnp.float32)
    conv_result = draw_conv_result(jax.random.fold_in(key_list[13], 71), 0)
    channel_norm_gain = jnp.clip(1.0 + 0.18 * jax.random.normal(key_list[12], (CONV_CHANNELS,), jnp.float32), 0.1, 1.9)
    return dict(stream_in=stream_in, out_cot=out_cot, route_experts=route_experts, route_weights=route_weights, w_gate=w_gate, w_up=w_up, w_down=w_down, w_proj=w_proj, conv_value=conv_value, conv_gate=conv_gate, conv_taps=conv_taps, conv_result=conv_result, channel_norm_gain=channel_norm_gain)


norm_eps = 1e-05
clamp_limit = 7.0
alpha_gate = 1.702

def slot_tables(block_routes, experts_all, capacity):
    flat_routes = block_routes.reshape(-1).astype(jnp.int32)
    assigns = flat_routes.shape[0]
    onehot = (flat_routes[:, None] == jnp.arange(experts_all, dtype=jnp.int32)[None, :]).astype(jnp.int32)
    before = jnp.cumsum(onehot, axis=0) - onehot
    rank_in = lax.optimization_barrier(jnp.sum(before * onehot, axis=1)).astype(jnp.int32)
    slot_of = (flat_routes * capacity + rank_in).astype(jnp.int32)
    source_of = jnp.full((experts_all * capacity,), -1, jnp.int32).at[slot_of].set(jnp.arange(assigns, dtype=jnp.int32))
    return (slot_of, source_of)

def one_expert(operands):
    rows_in, cot_in, gate_mat, up_mat, down_mat = operands
    pre_gate = jnp.dot(rows_in, gate_mat, preferred_element_type=jnp.float32)
    pre_up = jnp.dot(rows_in, up_mat, preferred_element_type=jnp.float32)
    glu_part = jnp.minimum(pre_gate, clamp_limit)
    lin_part = jnp.clip(pre_up, -clamp_limit, clamp_limit)
    sig_glu = jax.nn.sigmoid(alpha_gate * glu_part)
    activated = (glu_part * sig_glu * (lin_part + 1.0)).astype(jnp.bfloat16)
    grad_act = lax.dot_general(cot_in, down_mat, (((1,), (1,)), ((), ())), preferred_element_type=jnp.float32)
    slope = sig_glu + alpha_gate * glu_part * sig_glu * (1.0 - sig_glu)
    grad_pre_gate = jnp.where(pre_gate < clamp_limit, grad_act * (lin_part + 1.0) * slope, 0.0).astype(jnp.bfloat16)
    grad_pre_up = jnp.where(jnp.abs(pre_up) < clamp_limit, grad_act * glu_part * sig_glu, 0.0).astype(jnp.bfloat16)
    dims = (((0,), (0,)), ((), ()))
    grad_down = lax.dot_general(activated, cot_in, dims, preferred_element_type=jnp.float32).astype(jnp.bfloat16)
    grad_gate = lax.dot_general(rows_in, grad_pre_gate, dims, preferred_element_type=jnp.float32).astype(jnp.bfloat16)
    grad_up = lax.dot_general(rows_in, grad_pre_up, dims, preferred_element_type=jnp.float32).astype(jnp.bfloat16)
    row_count = rows_in.shape[0]
    group_width = FF // N_TP
    partial_sum = jnp.einsum('rpf,dpf->prd', grad_pre_gate.reshape(row_count, N_TP, group_width).astype(jnp.float32), gate_mat.reshape(D, N_TP, group_width).astype(jnp.float32))
    partial_sum = partial_sum + jnp.einsum('rpf,dpf->prd', grad_pre_up.reshape(row_count, N_TP, group_width).astype(jnp.float32), up_mat.reshape(D, N_TP, group_width).astype(jnp.float32))
    rounded = lax.optimization_barrier(partial_sum.astype(jnp.bfloat16))
    route_grad = lax.optimization_barrier(jnp.sum(rounded.astype(jnp.float32), axis=0)).astype(jnp.bfloat16)
    return (grad_gate, grad_up, grad_down, route_grad)

def reference(stream_in, out_cot, route_experts, route_weights, w_gate, w_up, w_down, w_proj, conv_value, conv_gate, conv_taps, conv_result, channel_norm_gain):
    block_routes = route_experts.reshape(N_SP, T_DEV, TOP)
    slot_of, source_of = jax.vmap(lambda routes_one: slot_tables(routes_one, EXPERTS, CAP))(block_routes)
    occupied = source_of >= 0
    source_safe = jnp.maximum(source_of, 0)
    offsets = (jnp.arange(N_SP, dtype=jnp.int32) * T_DEV)[:, None]
    token_of = (source_safe // TOP + offsets).astype(jnp.int32)
    weight_flat = route_weights.reshape(N_SP, T_DEV * TOP)
    slot_weight = jnp.where(occupied, jnp.take_along_axis(weight_flat, source_safe, axis=1), 0.0)
    row_buffer = jnp.where(occupied[..., None], stream_in[token_of], jnp.zeros((), jnp.bfloat16)).astype(jnp.bfloat16)
    cot_buffer = (slot_weight[..., None] * out_cot[token_of].astype(jnp.float32)).astype(jnp.bfloat16)
    row_buffer = row_buffer.reshape(N_SP, EXPERTS, CAP, D).transpose(1, 0, 2, 3).reshape(EXPERTS, N_SP * CAP, D)
    cot_buffer = cot_buffer.reshape(N_SP, EXPERTS, CAP, D).transpose(1, 0, 2, 3).reshape(EXPERTS, N_SP * CAP, D)
    grad_gate, grad_up, grad_down, route_grad = lax.map(one_expert, (row_buffer, cot_buffer, w_gate, w_up, w_down))
    returned = route_grad.reshape(EXPERTS, N_SP, CAP, D).transpose(1, 0, 2, 3).reshape(N_SP, EXPERTS * CAP, D)
    per_route = jnp.take_along_axis(returned, slot_of[..., None], axis=1).astype(jnp.float32)
    per_route = per_route.reshape(TOKENS, TOP, D)
    grad_stream = (out_cot.astype(jnp.float32) + lax.optimization_barrier(jnp.sum(per_route, axis=1))).astype(jnp.bfloat16)
    conv_float = conv_result.astype(jnp.float32)
    chan_mean = lax.optimization_barrier(jnp.sum(conv_float, axis=0)) / CONV_CHANNELS
    chan_var = lax.optimization_barrier(jnp.sum(conv_float * conv_float, axis=0)) / CONV_CHANNELS - chan_mean * chan_mean
    inverse_deviation = lax.rsqrt(chan_var + norm_eps)
    mean_removed = (conv_float - chan_mean) * inverse_deviation
    normalized_rows = mean_removed * channel_norm_gain[:, None]
    sigmoid_of_norm = jax.nn.sigmoid(normalized_rows)
    hidden = (normalized_rows * sigmoid_of_norm).astype(jnp.bfloat16)
    grad_proj = lax.dot_general(grad_stream, hidden, (((0,), (1,)), ((), ())), preferred_element_type=jnp.float32)
    hidden_gradient = lax.dot_general(w_proj, grad_stream, (((0,), (1,)), ((), ())), preferred_element_type=jnp.float32)
    normed_input_gradient = hidden_gradient * sigmoid_of_norm * (1.0 + normalized_rows * (1.0 - sigmoid_of_norm)) * channel_norm_gain[:, None]
    average_products = lax.optimization_barrier(jnp.sum(normed_input_gradient, axis=0)) / CONV_CHANNELS
    cross_products = lax.optimization_barrier(jnp.sum(normed_input_gradient * mean_removed, axis=0)) / CONV_CHANNELS
    conv_output_gradient = inverse_deviation * (normed_input_gradient - average_products - mean_removed * cross_products)
    extended = jnp.concatenate([conv_output_gradient, jnp.zeros((CONV_CHANNELS, CONV_W - 1), jnp.float32)], axis=1)
    grad_gated = jnp.zeros((CONV_CHANNELS, TOKENS), jnp.float32)
    for tap_index in range(CONV_W):
        grad_gated = grad_gated + conv_taps[tap_index][:, None] * extended[:, tap_index:tap_index + TOKENS]
    gate_sig = jax.nn.sigmoid(conv_gate.astype(jnp.float32))
    grad_value = (grad_gated * gate_sig).astype(jnp.bfloat16)
    grad_gate_in = (grad_gated * conv_value.astype(jnp.float32) * gate_sig * (1.0 - gate_sig)).astype(jnp.bfloat16)
    return (grad_gate, grad_up, grad_down, grad_stream, grad_proj, grad_value, grad_gate_in)
```

```python
import functools

import jax
import jax.numpy as jnp
from jax import lax
from jax.experimental import pallas as pl
from jax.experimental.pallas import tpu as pltpu
from jax.sharding import PartitionSpec as P

norm_eps = 1e-05
clamp_limit = 7.0
alpha_gate = 1.702
MESH = pl.DeviceIdType.MESH
f32 = jnp.float32
bf16 = jnp.bfloat16


def dot(a, b, ca=1, cb=0):
    return lax.dot_general(a, b, (((ca,), (cb,)), ((), ())), preferred_element_type=f32)


def aligned(start, size):
    return pl.ds(pl.multiple_of(start, size), size)


def greet(n, s, q, tp_peers):
    barrier = pltpu.get_barrier_semaphore()
    for d in range(1, n):
        pl.semaphore_signal(
            barrier, inc=1, device_id={"sp": lax.rem(s + d, n), "tp": q}, device_id_type=MESH
        )
    for peer in tp_peers:
        pl.semaphore_signal(barrier, inc=1, device_id={"sp": s, "tp": peer}, device_id_type=MESH)
    pl.semaphore_wait(barrier, n - 1 + len(tp_peers))


def remote(src, dst, send, recv, sp, tp):
    return pltpu.make_async_remote_copy(
        src_ref=src,
        dst_ref=dst,
        send_sem=send,
        recv_sem=recv,
        device_id={"sp": sp, "tp": tp},
        device_id_type=MESH,
    )


def partners(q):
    core, other = lax.rem(q, 2), q // 2
    return (2 * other + 1 - core, 2 * (1 - other) + core, 2 * (1 - other) + 1 - core)


def dispatch_kernel(
    n, cap, routes_ref, weights_ref, stream_ref, cot_ref, rows_ref, cots_ref, pick_ref,
    stage, send_xz, recv_xz, send_y, recv_y, send_c, recv_c, send_d, recv_d,
):
    s, q = lax.axis_index("sp"), lax.axis_index("tp")
    q_core, q_y, q_far = partners(q)
    top, tokens = routes_ref.shape
    width = stage.shape[-1]
    slots = pick_ref.shape[0]
    experts = slots // cap

    greet(n, s, q, (q_core, q_y))

    routes = routes_ref[...]
    expert_ids = lax.broadcasted_iota(jnp.int32, (experts, tokens), 0)
    hits = [expert_ids == routes[k : k + 1, :] for k in range(top)]
    count = sum(h.astype(f32) for h in hits)
    earlier = (
        lax.broadcasted_iota(jnp.int32, (tokens, tokens), 0)
        < lax.broadcasted_iota(jnp.int32, (tokens, tokens), 1)
    ).astype(f32)
    before = dot(count.astype(bf16), earlier.astype(bf16))
    slot_ids = lax.broadcasted_iota(jnp.int32, (slots, tokens), 0)
    pick = jnp.zeros((slots, tokens), f32)
    weighted = jnp.zeros((slots, tokens), f32)
    for k in range(top):
        rank = jnp.sum(jnp.where(hits[k], before, 0.0), axis=0, keepdims=True)
        slot = routes[k : k + 1, :] * cap + rank.astype(jnp.int32)
        here = slot_ids == slot
        pick = jnp.where(here, 1.0, pick)
        weighted = jnp.where(here, weights_ref[k : k + 1, :], weighted)
    slot_weight = jnp.sum(weighted, axis=1, keepdims=True)
    pick = pick.astype(bf16)
    pick_ref[...] = pick
    own = aligned(q * width, width)
    picked = dot(pick, stream_ref[:, own]).astype(bf16)
    stage[0] = picked
    stage[1] = (slot_weight * dot(pick, cot_ref[:, own])).astype(bf16)

    outs = (rows_ref, cots_ref)
    copies = []

    def start(copy):
        copy.start()
        copies.append(copy)
        return copy

    def at(a, source, quarter):
        return outs[a].at[aligned(source * cap, cap), aligned(quarter * width, width)]

    arriving = []
    for d in range(1, n):
        dest = lax.rem(s + d, n)
        arriving.append(
            [
                start(
                    remote(
                        stage.at[a, aligned(dest * cap, cap)], at(a, s, q),
                        send_xz.at[a, d], recv_xz.at[a, d], dest, q,
                    )
                )
                for a in range(2)
            ]
        )
    for a in range(2):
        outs[a][aligned(s * cap, cap), own] = stage[a, aligned(s * cap, cap), :]

    across, tail = [], []

    def far_forward(d):
        source = lax.rem(s + n - d, n)
        for a in range(2):
            across[d][a].wait_recv()
            tail.append(
                start(
                    remote(
                        at(a, source, q_y), at(a, source, q_y),
                        send_d.at[a, d], recv_d.at[a, d], s, q_core,
                    )
                )
            )

    for d in range(n):
        source = lax.rem(s + n - d, n)
        row = []
        for a in range(2):
            if d > 0:
                arriving[d - 1][a].wait_recv()
            block = at(a, source, q)
            row.append(start(remote(block, block, send_y.at[a, d], recv_y.at[a, d], s, q_y)))
            tail.append(start(remote(block, block, send_c.at[a, d], recv_c.at[a, d], s, q_core)))
        across.append(row)
        if d > 0:
            far_forward(d - 1)
    far_forward(n - 1)
    for copy in tail:
        copy.wait_recv()
    for copy in copies:
        copy.wait_send()


def dispatch(stream_in, out_cot, routes, weights, n, cap, tp_count, experts):
    tokens, model_width = stream_in.shape
    width = model_width // tp_count
    slots = experts * cap
    dma = [pltpu.SemaphoreType.DMA((2, n))] * 8
    return pl.pallas_call(
        functools.partial(dispatch_kernel, n, cap),
        out_shape=(
            jax.ShapeDtypeStruct((n * cap, model_width), bf16),
            jax.ShapeDtypeStruct((n * cap, model_width), bf16),
            jax.ShapeDtypeStruct((slots, tokens), bf16),
        ),
        in_specs=[pl.BlockSpec(memory_space=pltpu.VMEM)] * 4,
        out_specs=[pl.BlockSpec(memory_space=pltpu.VMEM)] * 3,
        scratch_shapes=[pltpu.VMEM((2, slots, width), bf16)] + dma,
        compiler_params=pltpu.CompilerParams(
            collective_id=0, has_side_effects=True, vmem_limit_bytes=24 << 20
        ),
        name="dispatch",
    )(routes, weights, stream_in, out_cot)


def tail_kernel(
    n, cap, channel_total,
    part_ref, pick_ref, cot_ref, proj_ref, value_ref, gate_ref, taps_ref, conv_ref, gain_ref,
    gs_ref, gproj_ref, gvalue_ref, ggate_ref,
    from_core, own, to_y, from_y, to_xz, ret, hid_all, col_all, stat, stat2, ext,
    send_c, recv_c, send_y, recv_y, send_r, recv_r, send_h, recv_h, send_s, recv_s,
    send_g, recv_g, send_k, recv_k, send_f, recv_f, send_e, recv_e,
):
    s, q = lax.axis_index("sp"), lax.axis_index("tp")
    q_core, q_y, q_far = partners(q)
    peers = (q_core, q_y, q_far)
    core, y = lax.rem(q, 2), q // 2
    tokens, model_width = gs_ref.shape
    width = ret.shape[-1]
    icols = gproj_ref.shape[0]
    taps_count = taps_ref.shape[0]
    copies = []

    def start(copy):
        copy.start()
        copies.append(copy)
        return copy

    greet(n, s, q, peers)

    order = [lax.rem(s + d, n) for d in range(1, n)] + [s]
    from_c = []
    for j, b in enumerate(order):
        rows = aligned(b * cap, cap)
        from_c.append(
            [
                start(
                    remote(
                        part_ref.at[rows, aligned((2 * half + 1 - core) * width, width)],
                        from_core.at[h, rows],
                        send_c.at[h, j], recv_c.at[h, j], s, q_core,
                    )
                )
                for h, half in ((0, 1 - y), (1, y))
            ]
        )

    def exchange_stats(buffer, first, second, which):
        lanes = lax.broadcasted_iota(jnp.int32, (tokens, tokens), 1)
        packed = jnp.where(lanes == 0, first, jnp.where(lanes == 1, second, 0.0))
        buffer[3] = packed.T[0:8, :]
        return [
            start(
                remote(
                    buffer.at[3], buffer.at[p], send_s.at[which, p], recv_s.at[which, p], s, peer
                )
            )
            for p, peer in enumerate(peers)
        ]

    def summed_stats(buffer, waits):
        for w in waits:
            w.wait_recv()
        total = (buffer[3] + buffer[0]) + (buffer[1] + buffer[2])
        wide = jnp.concatenate([total, jnp.zeros((tokens - 8, tokens), f32)], axis=0).T
        return wide[:, 0:1], wide[:, 1:2]

    conv = conv_ref[...].astype(f32).T
    stat_waits = exchange_stats(
        stat,
        jnp.sum(conv, axis=1, keepdims=True),
        jnp.sum(conv * conv, axis=1, keepdims=True),
        0,
    )
    over_y = []
    for j, b in enumerate(order):
        rows = aligned(b * cap, cap)
        from_c[j][0].wait_recv()
        to_y[rows, :] = (
            part_ref[rows, aligned((2 * (1 - y) + core) * width, width)].astype(f32)
            + from_core[0, rows, :].astype(f32)
        ).astype(bf16)
        over_y.append(
            start(
                remote(to_y.at[rows], from_y.at[rows], send_y.at[j], recv_y.at[j], s, q_y)
            )
        )
    for j, b in enumerate(order):
        rows = aligned(b * cap, cap)
        from_c[j][1].wait_recv()
        own[rows, :] = part_ref[rows, aligned(q * width, width)].astype(f32) + from_core[
            1, rows, :
        ].astype(f32)
    chan_sum, chan_sq = summed_stats(stat, stat_waits)
    chan_mean = chan_sum / channel_total
    chan_var = chan_sq / channel_total - chan_mean * chan_mean
    inverse_deviation = lax.rsqrt(chan_var + norm_eps)
    mean_removed = (conv - chan_mean) * inverse_deviation
    gain = gain_ref[...]
    normed = mean_removed * gain
    sig = jax.nn.sigmoid(normed)
    hid_all[aligned(s * tokens, tokens), :] = (normed * sig).astype(bf16)
    slope = sig * (1.0 + normed * (1.0 - sig)) * gain
    back = []
    for j, b in enumerate(order):
        rows = aligned(b * cap, cap)
        over_y[j].wait_recv()
        total = (own[rows, :] + from_y[rows, :].astype(f32)).astype(bf16)
        if j == n - 1:
            ret[rows, :] = total
        else:
            to_xz[rows, :] = total
            back.append(
                start(
                    remote(
                        to_xz.at[rows], ret.at[aligned(s * cap, cap)],
                        send_r.at[j], recv_r.at[j], b, q,
                    )
                )
            )
    mine = aligned(s * tokens, tokens)
    hid_waits = [
        start(
            remote(hid_all.at[mine], hid_all.at[mine], send_h.at[j], recv_h.at[j], order[j], q)
        )
        for j in range(n - 1)
    ]
    for copy in back:
        copy.wait_recv()
    quarter = aligned(q * width, width)
    combined = dot(pick_ref[...], ret[...], 0, 0) + cot_ref[:, quarter].astype(f32)
    gs_ref[:, quarter] = combined.astype(bf16)
    quarter_y = aligned(q_y * width, width)
    by_core = start(
        remote(gs_ref.at[:, quarter], gs_ref.at[:, quarter], send_g.at[0], recv_g.at[0], s, q_core)
    )
    by_y = start(
        remote(gs_ref.at[:, quarter], gs_ref.at[:, quarter], send_g.at[1], recv_g.at[1], s, q_y)
    )

    def partial_of(owner):
        cols = aligned(owner * width, width)
        return dot(gs_ref[:, cols], proj_ref[cols, :])

    grad_hidden = partial_of(q)
    by_y.wait_recv()
    by_far = start(
        remote(
            gs_ref.at[:, quarter_y], gs_ref.at[:, quarter_y], send_g.at[2], recv_g.at[2], s, q_core
        )
    )
    grad_hidden = grad_hidden + partial_of(q_y)
    by_core.wait_recv()
    grad_hidden = grad_hidden + partial_of(q_core)
    by_far.wait_recv()
    grad_hidden = grad_hidden + partial_of(q_far)
    half_rows = tokens // 2
    part_rows = aligned(core * half_rows, half_rows)
    land = aligned(s * tokens + core * half_rows, half_rows)
    col_waits = [
        start(
            remote(
                gs_ref.at[part_rows, aligned(order[j] * icols, icols)], col_all.at[land],
                send_k.at[j], recv_k.at[j], order[j], q,
            )
        )
        for j in range(n - 1)
    ]
    col_all[mine, :] = gs_ref[:, aligned(s * icols, icols)]
    norm_grad = grad_hidden * slope
    stat_waits = exchange_stats(
        stat2,
        jnp.sum(norm_grad, axis=1, keepdims=True),
        jnp.sum(norm_grad * mean_removed, axis=1, keepdims=True),
        1,
    )
    avg, cross = summed_stats(stat2, stat_waits)
    conv_grad = inverse_deviation * (
        norm_grad - avg / channel_total - mean_removed * (cross / channel_total)
    )
    rim = ext.shape[0] - tokens
    ext[0:tokens, :] = conv_grad
    halo = start(
        remote(
            ext.at[0:rim], ext.at[tokens : tokens + rim], send_e.at[0], recv_e.at[0],
            lax.rem(s + n - 1, n), q,
        )
    )
    forwards = []
    for j in range(n - 1):
        col_waits[j].wait_recv()
        source = lax.rem(s + n - (j + 1), n)
        there = aligned(source * tokens + core * half_rows, half_rows)
        forwards.append(
            start(
                remote(col_all.at[there], col_all.at[there], send_f.at[j], recv_f.at[j], s, q_core)
            )
        )
    halo.wait_recv()
    edge = ext[tokens : tokens + rim, :]
    halo.wait_send()
    ext[tokens : tokens + rim, :] = jnp.where(s == n - 1, 0.0, edge)
    acc = jnp.zeros((tokens, ext.shape[1]), f32)
    for tap in range(taps_count):
        acc = acc + taps_ref[tap : tap + 1, :] * ext[tap : tap + tokens, :]
    gated = acc.T
    gate_sig = jax.nn.sigmoid(gate_ref[...].astype(f32))
    gvalue_ref[...] = (gated * gate_sig).astype(bf16)
    ggate_ref[...] = (
        gated * value_ref[...].astype(f32) * gate_sig * (1.0 - gate_sig)
    ).astype(bf16)
    for copy in hid_waits + forwards:
        copy.wait_recv()
    gproj_ref[...] = dot(col_all[...], hid_all[...], 0, 0)
    for copy in copies:
        if copy is not halo:
            copy.wait_send()


def tail(part, pick, out_cot, w_proj, value, gate, taps, conv, gain, n, cap, tp_count):
    tokens, model_width = out_cot.shape
    width = model_width // tp_count
    channels = value.shape[0]
    icols = model_width // n
    slots = pick.shape[0]
    rows = part.shape[0]
    rim = -(-(taps.shape[0] - 1) // 8) * 8
    V = pltpu.VMEM
    dma = pltpu.SemaphoreType.DMA
    pairs = [(2, n), (n,), (n,), (n,), (2, 3), (3,), (n,), (n,), (1,)]
    return pl.pallas_call(
        functools.partial(tail_kernel, n, cap, channels * tp_count),
        out_shape=(
            jax.ShapeDtypeStruct((tokens, model_width), bf16),
            jax.ShapeDtypeStruct((icols, channels), f32),
            jax.ShapeDtypeStruct((channels, tokens), bf16),
            jax.ShapeDtypeStruct((channels, tokens), bf16),
        ),
        in_specs=[pl.BlockSpec(memory_space=V)] * 9,
        out_specs=[pl.BlockSpec(memory_space=V)] * 4,
        scratch_shapes=[
            V((2, rows, width), bf16),
            V((rows, width), f32),
            V((rows, width), bf16),
            V((rows, width), bf16),
            V((rows, width), bf16),
            V((slots, width), bf16),
            V((n * tokens, channels), bf16),
            V((n * tokens, icols), bf16),
            V((4, 8, tokens), f32),
            V((4, 8, tokens), f32),
            V((tokens + rim, channels), f32),
        ]
        + [dma(shape) for shape in pairs for _ in range(2)],
        compiler_params=pltpu.CompilerParams(
            collective_id=1, has_side_effects=True, vmem_limit_bytes=40 << 20
        ),
        name="combine_tail",
    )(part, pick, out_cot, w_proj, value, gate, taps, conv, gain)


def expert_terms(rows_in, cot_in, w_gate, w_up, w_down):
    pre_gate = dot(rows_in, w_gate)
    pre_up = dot(rows_in, w_up)
    glu_part = jnp.minimum(pre_gate, clamp_limit)
    lin_part = jnp.clip(pre_up, -clamp_limit, clamp_limit)
    sig_glu = jax.nn.sigmoid(alpha_gate * glu_part)
    activated = (glu_part * sig_glu * (lin_part + 1.0)).astype(bf16)
    grad_act = dot(cot_in, w_down, 1, 1)
    slope = sig_glu + alpha_gate * glu_part * sig_glu * (1.0 - sig_glu)
    grad_pre_gate = jnp.where(
        pre_gate < clamp_limit, grad_act * (lin_part + 1.0) * slope, 0.0
    ).astype(bf16)
    grad_pre_up = jnp.where(
        jnp.abs(pre_up) < clamp_limit, grad_act * glu_part * sig_glu, 0.0
    ).astype(bf16)
    grad_down = dot(activated, cot_in, 0, 0).astype(bf16)
    grad_gate = dot(rows_in, grad_pre_gate, 0, 0).astype(bf16)
    grad_up = dot(rows_in, grad_pre_up, 0, 0).astype(bf16)
    input_part = dot(grad_pre_gate, w_gate, 1, 1) + dot(grad_pre_up, w_up, 1, 1)
    return (grad_gate, grad_up, grad_down, input_part.astype(bf16))


def body(
    stream_in, out_cot, route_experts, route_weights, w_gate, w_up, w_down, w_proj,
    conv_value, conv_gate, conv_taps, conv_result, channel_norm_gain,
):
    n = lax.axis_size("sp")
    tp_count = lax.axis_size("tp")
    experts = w_gate.shape[0] * n
    tokens, model_width = stream_in.shape
    cap = 2 * route_experts.shape[1] * tokens // experts
    rows_in, cot_in, pick = dispatch(
        stream_in, out_cot, route_experts.T, route_weights.T, n, cap, tp_count, experts
    )
    grad_gate, grad_up, grad_down, part = expert_terms(
        rows_in, cot_in, w_gate[0], w_up[0], w_down[0]
    )
    grad_stream, grad_proj, grad_value, grad_gate_in = tail(
        part, pick, out_cot, w_proj, conv_value, conv_gate, conv_taps, conv_result,
        channel_norm_gain[None, :], n, cap, tp_count,
    )
    return (
        grad_gate[None], grad_up[None], grad_down[None],
        grad_stream, grad_proj, grad_value, grad_gate_in,
    )


def from_behind(value, axis, steps):
    count = lax.axis_size(axis)
    leading, last = (max(0, -steps), min(count, count - steps))
    return lax.ppermute(value, axis, [(source, source + steps) for source in range(leading, last)])


def slot_tables(block_routes, experts_all, capacity):
    flat_routes = block_routes.reshape(-1)
    assigns = flat_routes.shape[0]
    onehot = (flat_routes[:, None] == jnp.arange(experts_all, dtype=jnp.int32)[None, :]).astype(
        jnp.int32
    )
    before = jnp.cumsum(onehot, axis=0) - onehot
    rank_in = jnp.sum(before * onehot, axis=1)
    slot_of = flat_routes * capacity + rank_in
    source_of = (
        jnp.full((experts_all * capacity,), -1, jnp.int32)
        .at[slot_of]
        .set(jnp.arange(assigns, dtype=jnp.int32))
    )
    return (slot_of, source_of)


def combine_routes(returned, slot_of, cot_cols, token_rows, top_count):
    feature_count = returned.shape[-1]
    flat_back = returned.reshape(-1, feature_count)
    per_route = flat_back[slot_of].astype(jnp.float32).reshape(token_rows, top_count, feature_count)
    return (cot_cols.astype(jnp.float32) + jnp.sum(per_route, axis=1)).astype(jnp.bfloat16)


def expert_terms_plain(rows_in, cot_in, w_gate, w_up, w_down):
    pre_gate = jnp.einsum("secd,edf->secf", rows_in, w_gate, preferred_element_type=jnp.float32)
    pre_up = jnp.einsum("secd,edf->secf", rows_in, w_up, preferred_element_type=jnp.float32)
    glu_part = jnp.minimum(pre_gate, clamp_limit)
    lin_part = jnp.clip(pre_up, -clamp_limit, clamp_limit)
    sig_glu = jax.nn.sigmoid(alpha_gate * glu_part)
    activated = (glu_part * sig_glu * (lin_part + 1.0)).astype(jnp.bfloat16)
    grad_act = jnp.einsum("secd,efd->secf", cot_in, w_down, preferred_element_type=jnp.float32)
    slope = sig_glu + alpha_gate * glu_part * sig_glu * (1.0 - sig_glu)
    grad_pre_gate = jnp.where(
        pre_gate < clamp_limit, grad_act * (lin_part + 1.0) * slope, 0.0
    ).astype(jnp.bfloat16)
    grad_pre_up = jnp.where(
        jnp.abs(pre_up) < clamp_limit, grad_act * glu_part * sig_glu, 0.0
    ).astype(jnp.bfloat16)
    grad_down = jnp.einsum(
        "secf,secd->efd", activated, cot_in, preferred_element_type=jnp.float32
    ).astype(jnp.bfloat16)
    grad_gate = jnp.einsum(
        "secd,secf->edf", rows_in, grad_pre_gate, preferred_element_type=jnp.float32
    ).astype(jnp.bfloat16)
    grad_up = jnp.einsum(
        "secd,secf->edf", rows_in, grad_pre_up, preferred_element_type=jnp.float32
    ).astype(jnp.bfloat16)
    input_part = jnp.einsum(
        "secf,edf->secd", grad_pre_gate, w_gate, preferred_element_type=jnp.float32
    )
    input_part = input_part + jnp.einsum(
        "secf,edf->secd", grad_pre_up, w_up, preferred_element_type=jnp.float32
    )
    return (grad_gate, grad_up, grad_down, input_part)


def body_plain(
    stream_in,
    out_cot,
    route_experts,
    route_weights,
    w_gate,
    w_up,
    w_down,
    w_proj,
    conv_value,
    conv_gate,
    conv_taps,
    conv_result,
    channel_norm_gain,
):
    sp_count = lax.axis_size("sp")
    tp_count = lax.axis_size("tp")
    local_experts = w_gate.shape[0]
    experts_all = local_experts * sp_count
    token_rows, model_width = stream_in.shape
    top_count = route_experts.shape[1]
    capacity = 2 * top_count * token_rows // experts_all
    slot_of, source_of = slot_tables(route_experts, experts_all, capacity)
    occupied = source_of >= 0
    source_safe = jnp.maximum(source_of, 0)
    token_of = source_safe // top_count
    slot_weight = jnp.where(occupied, route_weights.reshape(-1)[source_safe], 0.0)
    row_buffer = jnp.where(occupied[:, None], stream_in[token_of], jnp.zeros((), jnp.bfloat16))
    cot_buffer = (slot_weight[:, None] * out_cot[token_of].astype(jnp.float32)).astype(jnp.bfloat16)
    row_buffer = row_buffer.reshape(experts_all, capacity, model_width)
    cot_buffer = cot_buffer.reshape(experts_all, capacity, model_width)
    slice_width = model_width // tp_count
    slice_start = lax.axis_index("tp") * slice_width
    row_slice = lax.dynamic_slice_in_dim(row_buffer, slice_start, slice_width, 2)
    cot_slice = lax.dynamic_slice_in_dim(cot_buffer, slice_start, slice_width, 2)
    row_slice, cot_slice = (
        lax.all_to_all(row_slice, "sp", split_axis=0, concat_axis=0, tiled=True),
        lax.all_to_all(cot_slice, "sp", split_axis=0, concat_axis=0, tiled=True),
    )
    rows_in, cot_in = (
        lax.all_gather(row_slice, "tp", axis=2, tiled=True),
        lax.all_gather(cot_slice, "tp", axis=2, tiled=True),
    )
    rows_in = rows_in.reshape(sp_count, local_experts, capacity, model_width)
    cot_in = cot_in.reshape(sp_count, local_experts, capacity, model_width)
    grad_gate, grad_up, grad_down, input_part = expert_terms_plain(rows_in, cot_in, w_gate, w_up, w_down)
    shared = lax.psum_scatter(
        input_part.astype(jnp.bfloat16), "tp", scatter_dimension=3, tiled=True
    )
    returned = shared.reshape(experts_all, capacity, slice_width)
    returned = lax.all_to_all(returned, "sp", split_axis=0, concat_axis=0, tiled=True)
    cot_cols = lax.dynamic_slice_in_dim(out_cot, slice_start, slice_width, 1)
    stream_part = combine_routes(returned, slot_of, cot_cols, token_rows, top_count)
    grad_stream = lax.all_gather(stream_part, "tp", axis=1, tiled=True)
    channel_total = conv_result.shape[0] * tp_count
    positions = conv_result.shape[1]
    conv_float = conv_result.astype(jnp.float32)
    chan_sum, chan_sq = lax.psum(
        (jnp.sum(conv_float, axis=0), jnp.sum(conv_float * conv_float, axis=0)), "tp"
    )
    chan_mean = chan_sum / channel_total
    chan_var = chan_sq / channel_total - chan_mean * chan_mean
    inverse_deviation = lax.rsqrt(chan_var + norm_eps)
    mean_removed = (conv_float - chan_mean) * inverse_deviation
    normalized_rows = mean_removed * channel_norm_gain[:, None]
    sigmoid_of_norm = jax.nn.sigmoid(normalized_rows)
    hidden = (normalized_rows * sigmoid_of_norm).astype(jnp.bfloat16)
    grad_proj = lax.psum_scatter(
        lax.dot_general(
            grad_stream, hidden, (((0,), (1,)), ((), ())), preferred_element_type=jnp.float32
        ),
        "sp",
        scatter_dimension=0,
        tiled=True,
    )
    hidden_gradient = lax.dot_general(
        w_proj, grad_stream, (((0,), (1,)), ((), ())), preferred_element_type=jnp.float32
    )
    normed_input_gradient = (
        hidden_gradient
        * sigmoid_of_norm
        * (1.0 + normalized_rows * (1.0 - sigmoid_of_norm))
        * channel_norm_gain[:, None]
    )
    average_products, cross_products = lax.psum(
        (
            jnp.sum(normed_input_gradient, axis=0),
            jnp.sum(normed_input_gradient * mean_removed, axis=0),
        ),
        "tp",
    )
    conv_output_gradient = inverse_deviation * (
        normed_input_gradient
        - average_products / channel_total
        - mean_removed * (cross_products / channel_total)
    )
    taps_count = conv_taps.shape[0]
    next_rim = from_behind(conv_output_gradient[:, : taps_count - 1], "sp", -1)
    extended = jnp.concatenate([conv_output_gradient, next_rim], axis=1)
    grad_gated = jnp.zeros_like(conv_output_gradient)
    for tap_index in range(taps_count):
        grad_gated = (
            grad_gated
            + conv_taps[tap_index][:, None] * extended[:, tap_index : tap_index + positions]
        )
    gate_sig = jax.nn.sigmoid(conv_gate.astype(jnp.float32))
    grad_value = (grad_gated * gate_sig).astype(jnp.bfloat16)
    grad_gate_in = (
        grad_gated * conv_value.astype(jnp.float32) * gate_sig * (1.0 - gate_sig)
    ).astype(jnp.bfloat16)
    return (grad_gate, grad_up, grad_down, grad_stream, grad_proj, grad_value, grad_gate_in)


def solution(mesh):
    return jax.shard_map(
        body if mesh.shape["tp"] == 4 else body_plain,
        mesh=mesh,
        in_specs=(
            P("sp", None),
            P("sp", None),
            P("sp", None),
            P("sp", None),
            P("sp", None, "tp"),
            P("sp", None, "tp"),
            P("sp", "tp", None),
            P(None, "tp"),
            P("tp", "sp"),
            P("tp", "sp"),
            P(None, "tp"),
            P("tp", "sp"),
            P("tp"),
        ),
        out_specs=(
            P("sp", None, "tp"),
            P("sp", None, "tp"),
            P("sp", "tp", None),
            P("sp", None),
            P("sp", "tp"),
            P("tp", "sp"),
            P("tp", "sp"),
        ),
        check_vma=False,
    )
```

```python
import functools

import jax
import jax.numpy as jnp
from jax import lax
from jax.experimental import pallas as pl
from jax.experimental.pallas import tpu as pltpu
from jax.sharding import PartitionSpec as P

norm_eps = 1e-05
clamp_limit = 7.0
alpha_gate = 1.702
MESH = pl.DeviceIdType.MESH
f32 = jnp.float32
bf16 = jnp.bfloat16


def dot(a, b, ca=1, cb=0):
    return lax.dot_general(a, b, (((ca,), (cb,)), ((), ())), preferred_element_type=f32)


def aligned(start, size):
    return pl.ds(pl.multiple_of(start, size), size)


def greet(n, s, q, tp_peers):
    barrier = pltpu.get_barrier_semaphore()
    for d in range(1, n):
        pl.semaphore_signal(
            barrier, inc=1, device_id={"sp": lax.rem(s + d, n), "tp": q}, device_id_type=MESH
        )
    for peer in tp_peers:
        pl.semaphore_signal(barrier, inc=1, device_id={"sp": s, "tp": peer}, device_id_type=MESH)
    pl.semaphore_wait(barrier, n - 1 + len(tp_peers))


def remote(src, dst, send, recv, sp, tp):
    return pltpu.make_async_remote_copy(
        src_ref=src,
        dst_ref=dst,
        send_sem=send,
        recv_sem=recv,
        device_id={"sp": sp, "tp": tp},
        device_id_type=MESH,
    )


def partners(q):
    core, other = lax.rem(q, 2), q // 2
    return (2 * other + 1 - core, 2 * (1 - other) + core, 2 * (1 - other) + 1 - core)


def dispatch_kernel(
    n, cap, routes_ref, weights_ref, stream_ref, cot_ref, rows_ref, cots_ref, pick_ref,
    weighted_ref, stage, send_xz, recv_xz, send_y, recv_y, send_c, recv_c, send_d, recv_d,
):
    s, q = lax.axis_index("sp"), lax.axis_index("tp")
    q_core, q_y, q_far = partners(q)
    top, tokens = routes_ref.shape
    width = stage.shape[-1]
    slots = pick_ref.shape[0]
    experts = slots // cap

    greet(n, s, q, (q_core, q_y))

    routes = routes_ref[...]
    expert_ids = lax.broadcasted_iota(jnp.int32, (experts, tokens), 0)
    hits = [expert_ids == routes[k : k + 1, :] for k in range(top)]
    count = sum(h.astype(f32) for h in hits)
    earlier = (
        lax.broadcasted_iota(jnp.int32, (tokens, tokens), 0)
        < lax.broadcasted_iota(jnp.int32, (tokens, tokens), 1)
    ).astype(f32)
    before = dot(count.astype(bf16), earlier.astype(bf16))
    slot_ids = lax.broadcasted_iota(jnp.int32, (slots, tokens), 0)
    pick = jnp.zeros((slots, tokens), f32)
    weighted = jnp.zeros((slots, tokens), f32)
    for k in range(top):
        rank = jnp.sum(jnp.where(hits[k], before, 0.0), axis=0, keepdims=True)
        slot = routes[k : k + 1, :] * cap + rank.astype(jnp.int32)
        here = slot_ids == slot
        pick = jnp.where(here, 1.0, pick)
        weighted = jnp.where(here, weights_ref[k : k + 1, :], weighted)
    slot_weight = jnp.sum(weighted, axis=1, keepdims=True)
    pick = pick.astype(bf16)
    pick_ref[...] = pick
    weighted_ref[...] = weighted
    own = aligned(q * width, width)
    picked = dot(pick, stream_ref[:, own]).astype(bf16)
    stage[0] = picked
    stage[1] = (slot_weight * dot(pick, cot_ref[:, own])).astype(bf16)

    outs = (rows_ref, cots_ref)
    copies = []

    def start(copy):
        copy.start()
        copies.append(copy)
        return copy

    def at(a, source, quarter):
        return outs[a].at[aligned(source * cap, cap), aligned(quarter * width, width)]

    arriving = []
    for d in range(1, n):
        dest = lax.rem(s + d, n)
        arriving.append(
            [
                start(
                    remote(
                        stage.at[a, aligned(dest * cap, cap)], at(a, s, q),
                        send_xz.at[a, d], recv_xz.at[a, d], dest, q,
                    )
                )
                for a in range(2)
            ]
        )
    mine = aligned(s * cap, cap)
    rows_ref[mine, :] = dot(pick_ref[mine, :], stream_ref[...]).astype(bf16)
    cots_ref[mine, :] = (
        jnp.sum(weighted_ref[mine, :], axis=1, keepdims=True)
        * dot(pick_ref[mine, :], cot_ref[...])
    ).astype(bf16)

    across, tail = [None], []

    def far_forward(d):
        source = lax.rem(s + n - d, n)
        for a in range(2):
            across[d][a].wait_recv()
            tail.append(
                start(
                    remote(
                        at(a, source, q_y), at(a, source, q_y),
                        send_d.at[a, d], recv_d.at[a, d], s, q_core,
                    )
                )
            )

    for d in range(1, n):
        source = lax.rem(s + n - d, n)
        row = []
        for a in range(2):
            arriving[d - 1][a].wait_recv()
            block = at(a, source, q)
            row.append(start(remote(block, block, send_y.at[a, d], recv_y.at[a, d], s, q_y)))
            tail.append(start(remote(block, block, send_c.at[a, d], recv_c.at[a, d], s, q_core)))
        across.append(row)
        if d > 1:
            far_forward(d - 1)
    far_forward(n - 1)
    for copy in tail:
        copy.wait_recv()
    for copy in copies:
        copy.wait_send()


def dispatch(stream_in, out_cot, routes, weights, n, cap, tp_count, experts):
    tokens, model_width = stream_in.shape
    width = model_width // tp_count
    slots = experts * cap
    dma = [pltpu.SemaphoreType.DMA((2, n))] * 8
    return pl.pallas_call(
        functools.partial(dispatch_kernel, n, cap),
        out_shape=(
            jax.ShapeDtypeStruct((n * cap, model_width), bf16),
            jax.ShapeDtypeStruct((n * cap, model_width), bf16),
            jax.ShapeDtypeStruct((slots, tokens), bf16),
        ),
        in_specs=[pl.BlockSpec(memory_space=pltpu.VMEM)] * 4,
        out_specs=[pl.BlockSpec(memory_space=pltpu.VMEM)] * 3,
        scratch_shapes=[
            pltpu.VMEM((slots, tokens), f32),
            pltpu.VMEM((2, slots, width), bf16),
        ]
        + dma,
        compiler_params=pltpu.CompilerParams(
            collective_id=0, has_side_effects=True, vmem_limit_bytes=24 << 20
        ),
        name="dispatch",
    )(routes, weights, stream_in, out_cot)


def tail_kernel(
    n, cap, channel_total,
    part_ref, pick_ref, cot_ref, proj_ref, value_ref, gate_ref, taps_ref, conv_ref, gain_ref,
    gs_ref, gproj_ref, gvalue_ref, ggate_ref,
    from_core, own, to_y, from_y, to_xz, ret, hid_all, col_all, stat, stat2, ext,
    send_c, recv_c, send_y, recv_y, send_r, recv_r, send_h, recv_h, send_s, recv_s,
    send_g, recv_g, send_k, recv_k, send_f, recv_f, send_e, recv_e,
):
    s, q = lax.axis_index("sp"), lax.axis_index("tp")
    q_core, q_y, q_far = partners(q)
    peers = (q_core, q_y, q_far)
    core, y = lax.rem(q, 2), q // 2
    tokens, model_width = gs_ref.shape
    width = ret.shape[-1]
    icols = gproj_ref.shape[0]
    taps_count = taps_ref.shape[0]
    copies = []

    def start(copy):
        copy.start()
        copies.append(copy)
        return copy

    greet(n, s, q, peers)

    order = [lax.rem(s + d, n) for d in range(1, n)] + [s]
    from_c = []
    for j, b in enumerate(order):
        rows = aligned(b * cap, cap)
        from_c.append(
            [
                start(
                    remote(
                        part_ref.at[rows, aligned((2 * half + 1 - core) * width, width)],
                        from_core.at[h, rows],
                        send_c.at[h, j], recv_c.at[h, j], s, q_core,
                    )
                )
                for h, half in ((0, 1 - y), (1, y))
            ]
        )

    def exchange_stats(buffer, first, second, which):
        lanes = lax.broadcasted_iota(jnp.int32, (tokens, tokens), 1)
        packed = jnp.where(lanes == 0, first, jnp.where(lanes == 1, second, 0.0))
        buffer[3] = packed.T[0:8, :]
        return [
            start(
                remote(
                    buffer.at[3], buffer.at[p], send_s.at[which, p], recv_s.at[which, p], s, peer
                )
            )
            for p, peer in enumerate(peers)
        ]

    def summed_stats(buffer, waits):
        for w in waits:
            w.wait_recv()
        total = (buffer[3] + buffer[0]) + (buffer[1] + buffer[2])
        wide = jnp.concatenate([total, jnp.zeros((tokens - 8, tokens), f32)], axis=0).T
        return wide[:, 0:1], wide[:, 1:2]

    conv = conv_ref[...].astype(f32).T
    stat_waits = exchange_stats(
        stat,
        jnp.sum(conv, axis=1, keepdims=True),
        jnp.sum(conv * conv, axis=1, keepdims=True),
        0,
    )
    over_y = []
    for j, b in enumerate(order):
        rows = aligned(b * cap, cap)
        from_c[j][0].wait_recv()
        to_y[rows, :] = (
            part_ref[rows, aligned((2 * (1 - y) + core) * width, width)].astype(f32)
            + from_core[0, rows, :].astype(f32)
        ).astype(bf16)
        over_y.append(
            start(
                remote(to_y.at[rows], from_y.at[rows], send_y.at[j], recv_y.at[j], s, q_y)
            )
        )
    for j, b in enumerate(order):
        rows = aligned(b * cap, cap)
        from_c[j][1].wait_recv()
        own[rows, :] = part_ref[rows, aligned(q * width, width)].astype(f32) + from_core[
            1, rows, :
        ].astype(f32)
    chan_sum, chan_sq = summed_stats(stat, stat_waits)
    chan_mean = chan_sum / channel_total
    chan_var = chan_sq / channel_total - chan_mean * chan_mean
    inverse_deviation = lax.rsqrt(chan_var + norm_eps)
    mean_removed = (conv - chan_mean) * inverse_deviation
    gain = gain_ref[...]
    normed = mean_removed * gain
    sig = jax.nn.sigmoid(normed)
    hid_all[aligned(s * tokens, tokens), :] = (normed * sig).astype(bf16)
    slope = sig * (1.0 + normed * (1.0 - sig)) * gain
    back = []
    for j, b in enumerate(order):
        rows = aligned(b * cap, cap)
        over_y[j].wait_recv()
        total = (own[rows, :] + from_y[rows, :].astype(f32)).astype(bf16)
        if j == n - 1:
            ret[rows, :] = total
        else:
            to_xz[rows, :] = total
            back.append(
                start(
                    remote(
                        to_xz.at[rows], ret.at[aligned(s * cap, cap)],
                        send_r.at[j], recv_r.at[j], b, q,
                    )
                )
            )
    mine = aligned(s * tokens, tokens)
    hid_waits = [
        start(
            remote(hid_all.at[mine], hid_all.at[mine], send_h.at[j], recv_h.at[j], order[j], q)
        )
        for j in range(n - 1)
    ]
    for copy in back:
        copy.wait_recv()
    quarter = aligned(q * width, width)
    combined = dot(pick_ref[...], ret[...], 0, 0) + cot_ref[:, quarter].astype(f32)
    gs_ref[:, quarter] = combined.astype(bf16)
    quarter_y = aligned(q_y * width, width)
    by_core = start(
        remote(gs_ref.at[:, quarter], gs_ref.at[:, quarter], send_g.at[0], recv_g.at[0], s, q_core)
    )
    by_y = start(
        remote(gs_ref.at[:, quarter], gs_ref.at[:, quarter], send_g.at[1], recv_g.at[1], s, q_y)
    )

    def partial_of(owner):
        cols = aligned(owner * width, width)
        return dot(gs_ref[:, cols], proj_ref[cols, :])

    grad_hidden = partial_of(q)
    by_y.wait_recv()
    by_far = start(
        remote(
            gs_ref.at[:, quarter_y], gs_ref.at[:, quarter_y], send_g.at[2], recv_g.at[2], s, q_core
        )
    )
    grad_hidden = grad_hidden + partial_of(q_y)
    by_core.wait_recv()
    grad_hidden = grad_hidden + partial_of(q_core)
    by_far.wait_recv()
    grad_hidden = grad_hidden + partial_of(q_far)
    half_rows = tokens // 2
    part_rows = aligned(core * half_rows, half_rows)
    land = aligned(s * tokens + core * half_rows, half_rows)
    col_waits = [
        start(
            remote(
                gs_ref.at[part_rows, aligned(order[j] * icols, icols)], col_all.at[land],
                send_k.at[j], recv_k.at[j], order[j], q,
            )
        )
        for j in range(n - 1)
    ]
    col_all[mine, :] = gs_ref[:, aligned(s * icols, icols)]
    norm_grad = grad_hidden * slope
    stat_waits = exchange_stats(
        stat2,
        jnp.sum(norm_grad, axis=1, keepdims=True),
        jnp.sum(norm_grad * mean_removed, axis=1, keepdims=True),
        1,
    )
    avg, cross = summed_stats(stat2, stat_waits)
    conv_grad = inverse_deviation * (
        norm_grad - avg / channel_total - mean_removed * (cross / channel_total)
    )
    rim = ext.shape[0] - tokens
    ext[0:tokens, :] = conv_grad
    halo = start(
        remote(
            ext.at[0:rim], ext.at[tokens : tokens + rim], send_e.at[0], recv_e.at[0],
            lax.rem(s + n - 1, n), q,
        )
    )
    forwards = []
    for j in range(n - 1):
        col_waits[j].wait_recv()
        source = lax.rem(s + n - (j + 1), n)
        there = aligned(source * tokens + core * half_rows, half_rows)
        forwards.append(
            start(
                remote(col_all.at[there], col_all.at[there], send_f.at[j], recv_f.at[j], s, q_core)
            )
        )
    halo.wait_recv()
    edge = ext[tokens : tokens + rim, :]
    halo.wait_send()
    ext[tokens : tokens + rim, :] = jnp.where(s == n - 1, 0.0, edge)
    acc = jnp.zeros((tokens, ext.shape[1]), f32)
    for tap in range(taps_count):
        acc = acc + taps_ref[tap : tap + 1, :] * ext[tap : tap + tokens, :]
    gated = acc.T
    gate_sig = jax.nn.sigmoid(gate_ref[...].astype(f32))
    gvalue_ref[...] = (gated * gate_sig).astype(bf16)
    ggate_ref[...] = (
        gated * value_ref[...].astype(f32) * gate_sig * (1.0 - gate_sig)
    ).astype(bf16)
    for copy in hid_waits + forwards:
        copy.wait_recv()
    gproj_ref[...] = dot(col_all[...], hid_all[...], 0, 0)
    for copy in copies:
        if copy is not halo:
            copy.wait_send()


def tail(part, pick, out_cot, w_proj, value, gate, taps, conv, gain, n, cap, tp_count):
    tokens, model_width = out_cot.shape
    width = model_width // tp_count
    channels = value.shape[0]
    icols = model_width // n
    slots = pick.shape[0]
    rows = part.shape[0]
    rim = -(-(taps.shape[0] - 1) // 8) * 8
    V = pltpu.VMEM
    dma = pltpu.SemaphoreType.DMA
    pairs = [(2, n), (n,), (n,), (n,), (2, 3), (3,), (n,), (n,), (1,)]
    return pl.pallas_call(
        functools.partial(tail_kernel, n, cap, channels * tp_count),
        out_shape=(
            jax.ShapeDtypeStruct((tokens, model_width), bf16),
            jax.ShapeDtypeStruct((icols, channels), f32),
            jax.ShapeDtypeStruct((channels, tokens), bf16),
            jax.ShapeDtypeStruct((channels, tokens), bf16),
        ),
        in_specs=[pl.BlockSpec(memory_space=V)] * 9,
        out_specs=[pl.BlockSpec(memory_space=V)] * 4,
        scratch_shapes=[
            V((2, rows, width), bf16),
            V((rows, width), f32),
            V((rows, width), bf16),
            V((rows, width), bf16),
            V((rows, width), bf16),
            V((slots, width), bf16),
            V((n * tokens, channels), bf16),
            V((n * tokens, icols), bf16),
            V((4, 8, tokens), f32),
            V((4, 8, tokens), f32),
            V((tokens + rim, channels), f32),
        ]
        + [dma(shape) for shape in pairs for _ in range(2)],
        compiler_params=pltpu.CompilerParams(
            collective_id=1, has_side_effects=True, vmem_limit_bytes=40 << 20
        ),
        name="combine_tail",
    )(part, pick, out_cot, w_proj, value, gate, taps, conv, gain)


def flush_kernel(*refs):
    count = len(refs) // 2
    copies = [
        pltpu.make_async_copy(refs[i], refs[count + i], refs[-1].at[i]) for i in range(count)
    ]
    for copy in copies:
        copy.start()
    for copy in copies:
        copy.wait()


def flush(*arrays):
    return pl.pallas_call(
        flush_kernel,
        out_shape=tuple(jax.ShapeDtypeStruct(a.shape, a.dtype) for a in arrays),
        in_specs=[pl.BlockSpec(memory_space=pltpu.VMEM)] * len(arrays),
        out_specs=[pl.BlockSpec(memory_space=pltpu.HBM)] * len(arrays),
        scratch_shapes=[pltpu.SemaphoreType.DMA((len(arrays),))],
        compiler_params=pltpu.CompilerParams(vmem_limit_bytes=4 << 20),
        name="flush",
    )(*arrays)


def expert_terms(rows_in, cot_in, w_gate, w_up, w_down):
    pre_gate = dot(rows_in, w_gate)
    pre_up = dot(rows_in, w_up)
    glu_part = jnp.minimum(pre_gate, clamp_limit)
    lin_part = jnp.clip(pre_up, -clamp_limit, clamp_limit)
    sig_glu = jax.nn.sigmoid(alpha_gate * glu_part)
    activated = (glu_part * sig_glu * (lin_part + 1.0)).astype(bf16)
    grad_act = dot(cot_in, w_down, 1, 1)
    slope = sig_glu + alpha_gate * glu_part * sig_glu * (1.0 - sig_glu)
    grad_pre_gate = jnp.where(
        pre_gate < clamp_limit, grad_act * (lin_part + 1.0) * slope, 0.0
    ).astype(bf16)
    grad_pre_up = jnp.where(
        jnp.abs(pre_up) < clamp_limit, grad_act * glu_part * sig_glu, 0.0
    ).astype(bf16)
    grad_down = dot(activated, cot_in, 0, 0).astype(bf16)
    grad_gate = dot(rows_in, grad_pre_gate, 0, 0).astype(bf16)
    grad_up = dot(rows_in, grad_pre_up, 0, 0).astype(bf16)
    input_part = dot(grad_pre_gate, w_gate, 1, 1) + dot(grad_pre_up, w_up, 1, 1)
    return (grad_gate, grad_up, grad_down, input_part.astype(bf16))


def body(
    stream_in, out_cot, route_experts, route_weights, w_gate, w_up, w_down, w_proj,
    conv_value, conv_gate, conv_taps, conv_result, channel_norm_gain,
):
    n = lax.axis_size("sp")
    tp_count = lax.axis_size("tp")
    experts = w_gate.shape[0] * n
    tokens, model_width = stream_in.shape
    cap = 2 * route_experts.shape[1] * tokens // experts
    rows_in, cot_in, pick = dispatch(
        stream_in, out_cot, route_experts.T, route_weights.T, n, cap, tp_count, experts
    )
    grad_gate, grad_up, grad_down, part = expert_terms(
        rows_in, cot_in, w_gate[0], w_up[0], w_down[0]
    )
    grad_stream, grad_proj, grad_value, grad_gate_in = tail(
        part, pick, out_cot, w_proj, conv_value, conv_gate, conv_taps, conv_result,
        channel_norm_gain[None, :], n, cap, tp_count,
    )
    grad_stream, grad_proj, grad_value, grad_gate_in = flush(
        grad_stream, grad_proj, grad_value, grad_gate_in
    )
    return (
        grad_gate[None], grad_up[None], grad_down[None],
        grad_stream, grad_proj, grad_value, grad_gate_in,
    )


def from_behind(value, axis, steps):
    count = lax.axis_size(axis)
    leading, last = (max(0, -steps), min(count, count - steps))
    return lax.ppermute(value, axis, [(source, source + steps) for source in range(leading, last)])


def slot_tables(block_routes, experts_all, capacity):
    flat_routes = block_routes.reshape(-1)
    assigns = flat_routes.shape[0]
    onehot = (flat_routes[:, None] == jnp.arange(experts_all, dtype=jnp.int32)[None, :]).astype(
        jnp.int32
    )
    before = jnp.cumsum(onehot, axis=0) - onehot
    rank_in = jnp.sum(before * onehot, axis=1)
    slot_of = flat_routes * capacity + rank_in
    source_of = (
        jnp.full((experts_all * capacity,), -1, jnp.int32)
        .at[slot_of]
        .set(jnp.arange(assigns, dtype=jnp.int32))
    )
    return (slot_of, source_of)


def combine_routes(returned, slot_of, cot_cols, token_rows, top_count):
    feature_count = returned.shape[-1]
    flat_back = returned.reshape(-1, feature_count)
    per_route = flat_back[slot_of].astype(jnp.float32).reshape(token_rows, top_count, feature_count)
    return (cot_cols.astype(jnp.float32) + jnp.sum(per_route, axis=1)).astype(jnp.bfloat16)


def expert_terms_plain(rows_in, cot_in, w_gate, w_up, w_down):
    pre_gate = jnp.einsum("secd,edf->secf", rows_in, w_gate, preferred_element_type=jnp.float32)
    pre_up = jnp.einsum("secd,edf->secf", rows_in, w_up, preferred_element_type=jnp.float32)
    glu_part = jnp.minimum(pre_gate, clamp_limit)
    lin_part = jnp.clip(pre_up, -clamp_limit, clamp_limit)
    sig_glu = jax.nn.sigmoid(alpha_gate * glu_part)
    activated = (glu_part * sig_glu * (lin_part + 1.0)).astype(jnp.bfloat16)
    grad_act = jnp.einsum("secd,efd->secf", cot_in, w_down, preferred_element_type=jnp.float32)
    slope = sig_glu + alpha_gate * glu_part * sig_glu * (1.0 - sig_glu)
    grad_pre_gate = jnp.where(
        pre_gate < clamp_limit, grad_act * (lin_part + 1.0) * slope, 0.0
    ).astype(jnp.bfloat16)
    grad_pre_up = jnp.where(
        jnp.abs(pre_up) < clamp_limit, grad_act * glu_part * sig_glu, 0.0
    ).astype(jnp.bfloat16)
    grad_down = jnp.einsum(
        "secf,secd->efd", activated, cot_in, preferred_element_type=jnp.float32
    ).astype(jnp.bfloat16)
    grad_gate = jnp.einsum(
        "secd,secf->edf", rows_in, grad_pre_gate, preferred_element_type=jnp.float32
    ).astype(jnp.bfloat16)
    grad_up = jnp.einsum(
        "secd,secf->edf", rows_in, grad_pre_up, preferred_element_type=jnp.float32
    ).astype(jnp.bfloat16)
    input_part = jnp.einsum(
        "secf,edf->secd", grad_pre_gate, w_gate, preferred_element_type=jnp.float32
    )
    input_part = input_part + jnp.einsum(
        "secf,edf->secd", grad_pre_up, w_up, preferred_element_type=jnp.float32
    )
    return (grad_gate, grad_up, grad_down, input_part)


def body_plain(
    stream_in,
    out_cot,
    route_experts,
    route_weights,
    w_gate,
    w_up,
    w_down,
    w_proj,
    conv_value,
    conv_gate,
    conv_taps,
    conv_result,
    channel_norm_gain,
):
    sp_count = lax.axis_size("sp")
    tp_count = lax.axis_size("tp")
    local_experts = w_gate.shape[0]
    experts_all = local_experts * sp_count
    token_rows, model_width = stream_in.shape
    top_count = route_experts.shape[1]
    capacity = 2 * top_count * token_rows // experts_all
    slot_of, source_of = slot_tables(route_experts, experts_all, capacity)
    occupied = source_of >= 0
    source_safe = jnp.maximum(source_of, 0)
    token_of = source_safe // top_count
    slot_weight = jnp.where(occupied, route_weights.reshape(-1)[source_safe], 0.0)
    row_buffer = jnp.where(occupied[:, None], stream_in[token_of], jnp.zeros((), jnp.bfloat16))
    cot_buffer = (slot_weight[:, None] * out_cot[token_of].astype(jnp.float32)).astype(jnp.bfloat16)
    row_buffer = row_buffer.reshape(experts_all, capacity, model_width)
    cot_buffer = cot_buffer.reshape(experts_all, capacity, model_width)
    slice_width = model_width // tp_count
    slice_start = lax.axis_index("tp") * slice_width
    row_slice = lax.dynamic_slice_in_dim(row_buffer, slice_start, slice_width, 2)
    cot_slice = lax.dynamic_slice_in_dim(cot_buffer, slice_start, slice_width, 2)
    row_slice, cot_slice = (
        lax.all_to_all(row_slice, "sp", split_axis=0, concat_axis=0, tiled=True),
        lax.all_to_all(cot_slice, "sp", split_axis=0, concat_axis=0, tiled=True),
    )
    rows_in, cot_in = (
        lax.all_gather(row_slice, "tp", axis=2, tiled=True),
        lax.all_gather(cot_slice, "tp", axis=2, tiled=True),
    )
    rows_in = rows_in.reshape(sp_count, local_experts, capacity, model_width)
    cot_in = cot_in.reshape(sp_count, local_experts, capacity, model_width)
    grad_gate, grad_up, grad_down, input_part = expert_terms_plain(rows_in, cot_in, w_gate, w_up, w_down)
    shared = lax.psum_scatter(
        input_part.astype(jnp.bfloat16), "tp", scatter_dimension=3, tiled=True
    )
    returned = shared.reshape(experts_all, capacity, slice_width)
    returned = lax.all_to_all(returned, "sp", split_axis=0, concat_axis=0, tiled=True)
    cot_cols = lax.dynamic_slice_in_dim(out_cot, slice_start, slice_width, 1)
    stream_part = combine_routes(returned, slot_of, cot_cols, token_rows, top_count)
    grad_stream = lax.all_gather(stream_part, "tp", axis=1, tiled=True)
    channel_total = conv_result.shape[0] * tp_count
    positions = conv_result.shape[1]
    conv_float = conv_result.astype(jnp.float32)
    chan_sum, chan_sq = lax.psum(
        (jnp.sum(conv_float, axis=0), jnp.sum(conv_float * conv_float, axis=0)), "tp"
    )
    chan_mean = chan_sum / channel_total
    chan_var = chan_sq / channel_total - chan_mean * chan_mean
    inverse_deviation = lax.rsqrt(chan_var + norm_eps)
    mean_removed = (conv_float - chan_mean) * inverse_deviation
    normalized_rows = mean_removed * channel_norm_gain[:, None]
    sigmoid_of_norm = jax.nn.sigmoid(normalized_rows)
    hidden = (normalized_rows * sigmoid_of_norm).astype(jnp.bfloat16)
    grad_proj = lax.psum_scatter(
        lax.dot_general(
            grad_stream, hidden, (((0,), (1,)), ((), ())), preferred_element_type=jnp.float32
        ),
        "sp",
        scatter_dimension=0,
        tiled=True,
    )
    hidden_gradient = lax.dot_general(
        w_proj, grad_stream, (((0,), (1,)), ((), ())), preferred_element_type=jnp.float32
    )
    normed_input_gradient = (
        hidden_gradient
        * sigmoid_of_norm
        * (1.0 + normalized_rows * (1.0 - sigmoid_of_norm))
        * channel_norm_gain[:, None]
    )
    average_products, cross_products = lax.psum(
        (
            jnp.sum(normed_input_gradient, axis=0),
            jnp.sum(normed_input_gradient * mean_removed, axis=0),
        ),
        "tp",
    )
    conv_output_gradient = inverse_deviation * (
        normed_input_gradient
        - average_products / channel_total
        - mean_removed * (cross_products / channel_total)
    )
    taps_count = conv_taps.shape[0]
    next_rim = from_behind(conv_output_gradient[:, : taps_count - 1], "sp", -1)
    extended = jnp.concatenate([conv_output_gradient, next_rim], axis=1)
    grad_gated = jnp.zeros_like(conv_output_gradient)
    for tap_index in range(taps_count):
        grad_gated = (
            grad_gated
            + conv_taps[tap_index][:, None] * extended[:, tap_index : tap_index + positions]
        )
    gate_sig = jax.nn.sigmoid(conv_gate.astype(jnp.float32))
    grad_value = (grad_gated * gate_sig).astype(jnp.bfloat16)
    grad_gate_in = (
        grad_gated * conv_value.astype(jnp.float32) * gate_sig * (1.0 - gate_sig)
    ).astype(jnp.bfloat16)
    return (grad_gate, grad_up, grad_down, grad_stream, grad_proj, grad_value, grad_gate_in)


def solution(mesh):
    return jax.shard_map(
        body if mesh.shape["tp"] == 4 else body_plain,
        mesh=mesh,
        in_specs=(
            P("sp", None),
            P("sp", None),
            P("sp", None),
            P("sp", None),
            P("sp", None, "tp"),
            P("sp", None, "tp"),
            P("sp", "tp", None),
            P(None, "tp"),
            P("tp", "sp"),
            P("tp", "sp"),
            P(None, "tp"),
            P("tp", "sp"),
            P("tp"),
        ),
        out_specs=(
            P("sp", None, "tp"),
            P("sp", None, "tp"),
            P("sp", "tp", None),
            P("sp", None),
            P("sp", "tp"),
            P("tp", "sp"),
            P("tp", "sp"),
        ),
        check_vma=False,
    )
```
